32 devices in a mesh: rep: 2 (over y), fs: 4 (over z), tp: 4 (over x, core).
Axes of the slice: x: 2, y: 2, z: 4, core: 2. Of those that a mesh axis runs over, the one named last changes fastest.
Arguments:
- stream: bfloat16 [4096, 2048], P(('rep', 'fs'), 'tp'), parts along dimension 0, may hold values from -6 to 6
- in_weight: bfloat16 [2048, 1024], P('fs', 'tp'), may hold values from -0.125 to 0.125
- pool_weight: bfloat16 [8, 128, 128], P('tp'), may hold values from -0.5 to 0.5
- pool_scale: bfloat16 [1024], P('tp'), may hold values from 0.099609375 to 1.8984375
- out_weight: bfloat16 [1024, 2048], P('tp', 'fs'), may hold values from -0.1875 to 0.1875
- mix_gain: bfloat16 [2048], replicated, may hold values from 0.099609375 to 1.8984375
- ffn_gain: bfloat16 [2048], replicated, may hold values from 0.099609375 to 1.8984375
- gate_weight: bfloat16 [2048, 5632], P('fs', 'tp'), may hold values from -0.125 to 0.125
- up_weight: bfloat16 [2048, 5632], P('fs', 'tp'), may hold values from -0.125 to 0.125
- down_weight: bfloat16 [5632, 2048], P('tp', 'fs'), may hold values from -0.078125 to 0.078125
Outputs:
- result: bfloat16 [4096, 2048], P(('rep', 'fs'), 'tp'), parts along dimension 0
The draws below stay inside these ranges and needn't reach their ends.
There are 2 independent parts, one for each index of `rep`. The reference program is written for one: setup_inputs(seed, part) draws one part's arguments, and reference() takes and returns one part's arrays. A program takes and returns all parts, laid end to end along the dimension named above; an argument that names none is the same for every part. Nothing has to cross between parts.
All inputs are finite; a program needn't handle non-finite values.
Results may differ from the reference program's by a relative error of at most 0.015.
Values may be sent and summed in bfloat16 or wider, within the bound.
No kernel may reach another device: no remote copies, remote signals or barrier semaphores. Data moves between devices by JAX's collectives and lax.ppermute only.
A program may use at most 64 MiB of HBM per device.

```python
import jax
import jax.numpy as jnp
from jax import lax

D = 2048
GROUPS = 8
GROUP_DIM = 128
FF = 5632
SEQ = 128
POOL_CH = 1024
TOKENS = 2048
N_TP = 4


def block_scale(own_key, shape, split, least, high):
    factor_of, own = 1.0, jax.random.fold_in(own_key, 6)
    for axis_at, parts in split:
        steps = jnp.exp(jax.random.uniform(jax.random.fold_in(own, axis_at), (parts,), jnp.float32, least / len(split), high / len(split)))
        factor_of = factor_of * jnp.repeat(steps, shape[axis_at] // parts).reshape([-1 if axis == axis_at else 1 for axis in range(len(shape))])
    return factor_of


def bell_draw(rng, extent, width, bound, cuts=(), kind=jnp.bfloat16):
    array = width * jax.random.normal(rng, extent, jnp.float32)
    if cuts:
        array = array * block_scale(rng, extent, cuts, -0.22, 0.18)
    return jnp.clip(array, -bound, bound).astype(kind)


def setup_inputs(seed: int = 0, part: int = 0) -> dict:
    keys = jax.random.split(jax.random.key(seed), 11)
    part_keys = jax.random.split(jax.random.fold_in(keys[10], part), 11)
    return {
        "stream": bell_draw(part_keys[0], (TOKENS, D), 1.0, 6.0, ((0, 4), (1, 4))),
        "in_weight": bell_draw(keys[1], (D, POOL_CH), D ** -0.5, 0.125, ((0, 4), (1, 4))),
        "pool_weight": bell_draw(keys[2], (GROUPS, GROUP_DIM, GROUP_DIM), GROUP_DIM ** -0.5, 0.5, ((0, 4),)),
        "pool_scale": jnp.clip(1.0 + 0.18 * jax.random.normal(keys[3], (POOL_CH,), jnp.float32), 0.099609375, 1.8984375).astype(jnp.bfloat16),
        "out_weight": bell_draw(keys[4], (POOL_CH, D), POOL_CH ** -0.5, 0.1875, ((0, 4), (1, 4))),
        "mix_gain": jnp.clip(1.0 + 0.18 * jax.random.normal(keys[5], (D,), jnp.float32), 0.099609375, 1.8984375).astype(jnp.bfloat16),
        "ffn_gain": jnp.clip(1.0 + 0.18 * jax.random.normal(keys[6], (D,), jnp.float32), 0.099609375, 1.8984375).astype(jnp.bfloat16),
        "gate_weight": bell_draw(keys[7], (D, FF), D ** -0.5, 0.125, ((0, 4), (1, 4))),
        "up_weight": bell_draw(keys[8], (D, FF), D ** -0.5, 0.125, ((0, 4), (1, 4))),
        "down_weight": bell_draw(keys[9], (FF, D), FF ** -0.5, 0.078125, ((0, 4), (1, 4))),
    }


epsilon = 1e-06

def root_norm(values, gain_vec):
    widened = values.astype(jnp.float32)
    scaled = widened * lax.rsqrt(lax.optimization_barrier(jnp.mean(widened * widened, axis=-1, keepdims=True)) + epsilon)
    return (scaled * gain_vec.astype(jnp.float32)).astype(jnp.bfloat16)

def window_tables(first_group, group_count, seq_len, total_groups):
    group_ids = first_group + jnp.arange(group_count, dtype=jnp.int32)
    reaches = jnp.left_shift(jnp.int32(2), 4 * group_ids // total_groups)
    query_pos = jnp.arange(seq_len, dtype=jnp.int32)[:, None]
    earlier = jnp.arange(seq_len, dtype=jnp.int32)[None, :]
    inside = (earlier <= query_pos)[None] & (earlier[None] > query_pos[None] - reaches[:, None, None])
    counts = jnp.minimum(query_pos[:, 0][None, :] + 1, reaches[:, None]).astype(jnp.float32)
    return (inside, counts)

def block_sum(operand, weights):
    block_width = operand.shape[1] // N_TP
    running = jnp.zeros((operand.shape[0], weights.shape[1]), jnp.float32)
    for block_id in range(N_TP):
        product = jnp.dot(operand[:, block_id * block_width:(block_id + 1) * block_width], weights[block_id * block_width:(block_id + 1) * block_width], preferred_element_type=jnp.float32)
        rounded = lax.optimization_barrier(product.astype(jnp.bfloat16))
        running = running + rounded.astype(jnp.float32)
    return running

def reference(stream, in_weight, pool_weight, pool_scale, out_weight, mix_gain, ffn_gain, gate_weight, up_weight, down_weight):
    normed = root_norm(stream, mix_gain)
    pooled_in = jnp.dot(normed, in_weight, preferred_element_type=jnp.float32).astype(jnp.bfloat16)
    inside, counts = window_tables(0, GROUPS, SEQ, GROUPS)
    grouped = pooled_in.astype(jnp.float32).reshape(TOKENS // SEQ, SEQ, GROUPS, GROUP_DIM)
    window_sums = jnp.einsum('gts,nsgc->ntgc', inside.astype(jnp.float32), grouped, precision=lax.Precision.HIGHEST)
    contrast = (window_sums / counts.T[None, :, :, None] - grouped).astype(jnp.bfloat16)
    mixed_out = jnp.einsum('ntgc,gcd->ntgd', contrast.astype(jnp.float32), pool_weight.astype(jnp.float32))
    group_out = (mixed_out.reshape(TOKENS, POOL_CH) * pool_scale.astype(jnp.float32)).astype(jnp.bfloat16)
    mixer_sum = block_sum(group_out, out_weight)
    middle = (stream.astype(jnp.float32) + mixer_sum).astype(jnp.bfloat16)
    normed_ffn = root_norm(middle, ffn_gain)
    gate_acts = jnp.dot(normed_ffn, gate_weight, preferred_element_type=jnp.float32)
    up_acts = jnp.dot(normed_ffn, up_weight, preferred_element_type=jnp.float32)
    hidden = (jax.nn.silu(gate_acts) * up_acts).astype(jnp.bfloat16)
    ffn_sum = block_sum(hidden, down_weight)
    return (middle.astype(jnp.float32) + ffn_sum).astype(jnp.bfloat16)
```

```python
import jax
import jax.numpy as jnp
from jax import lax
from jax.sharding import PartitionSpec as P

GROUPS = 8
SEQ = 128
MAX_SENDS = 8
epsilon = 1e-06


def swap(values, axis, mask):
    return lax.ppermute(values, axis, [(i, i ^ mask) for i in range(lax.axis_size(axis))])


def regroup(values, mask, inverse):
    tp, fs = lax.axis_size("tp"), lax.axis_size("fs")
    edges = []
    for z in range(fs):
        for t in range(tp):
            to_z = (z & ~1) | ((t & 1) ^ (mask & 1))
            to_t = (((t >> 1) ^ (mask >> 1)) << 1) | (z & 1)
            edge = (z * tp + t, to_z * tp + to_t)
            edges.append(edge[::-1] if inverse else edge)
    return lax.ppermute(values, ("fs", "tp"), edges)


def put(buffer, piece, index):
    lead = len(index)
    piece = piece.reshape((1,) * lead + buffer.shape[lead:])
    return lax.dynamic_update_slice(buffer, piece, tuple(index) + (0,) * (buffer.ndim - lead))


def part(values, index, count):
    rows = values.shape[0] // count
    return lax.dynamic_slice_in_dim(values, index * rows, rows, axis=0)


def gather_planes(shard):
    fs, rep = lax.axis_size("fs"), lax.axis_size("rep")
    z, r = lax.axis_index("fs"), lax.axis_index("rep")
    if fs > MAX_SENDS:
        return lax.all_gather(shard, "fs")
    rows = shard.shape[0] // rep
    mine = part(shard, r, rep)
    local = shard.reshape((1, rep, rows, shard.shape[1]))
    buffer = jnp.broadcast_to(local, (fs,) + local.shape[1:])
    for s in range(1, fs):
        got = swap(mine, "fs", s)
        for q in range(rep):
            buffer = put(buffer, got if q == 0 else swap(got, "rep", q), (z ^ s, r ^ q))
    return buffer.reshape(fs, shard.shape[0], shard.shape[1])


def gather_hidden(shard):
    fs, rep = lax.axis_size("fs"), lax.axis_size("rep")
    z, r = lax.axis_index("fs"), lax.axis_index("rep")
    c = lax.axis_index("tp") & 1
    same_core = c == (z & 1)
    rows = shard.shape[0] // (2 * rep)
    other = swap(shard, "tp", 1)
    own_part, other_part = part(shard, c * rep + r, 2 * rep), part(other, c * rep + r, 2 * rep)
    even = jnp.where(same_core, own_part, other_part)
    odd = jnp.where(same_core, other_part, own_part)
    if fs > MAX_SENDS:
        sends = jnp.stack([odd if s & 1 else even for s in range(fs)])
        sends = jnp.where((z & 1) == 0, sends, jnp.roll(sends, 1, axis=0))
        got = lax.all_to_all(sends, "fs", 0, 0, tiled=True)
        got = lax.all_gather(got, "rep", axis=1)
        both = jnp.stack([got, swap(got, "tp", 1)], axis=1)
        both = jnp.where(c == 0, both, jnp.roll(both, 1, axis=1))
        return both.reshape(fs, shard.shape[0], shard.shape[1])
    local = jnp.where(same_core, shard, other).reshape((1, 2, rep, rows, shard.shape[1]))
    buffer = jnp.broadcast_to(local, (fs,) + local.shape[1:])
    for s in range(1, fs):
        got = swap(odd if s & 1 else even, "fs", s)
        for q in range(rep):
            piece = got if q == 0 else swap(got, "rep", q)
            buffer = put(buffer, piece, (z ^ s, c, r ^ q))
            buffer = put(buffer, swap(piece, "tp", 1), (z ^ s, c ^ 1, r ^ q))
    return buffer.reshape(fs, shard.shape[0], shard.shape[1])


def window_tables(first_group, group_count, seq_len, total_groups):
    group_ids = first_group + jnp.arange(group_count, dtype=jnp.int32)
    reaches = jnp.left_shift(jnp.int32(2), 4 * group_ids // total_groups)
    query_pos = jnp.arange(seq_len, dtype=jnp.int32)[:, None]
    earlier = jnp.arange(seq_len, dtype=jnp.int32)[None, :]
    inside = (earlier <= query_pos)[None] & (
        earlier[None] > query_pos[None] - reaches[:, None, None]
    )
    counts = jnp.minimum(query_pos[:, 0][None, :] + 1, reaches[:, None]).astype(jnp.float32)
    return (inside, counts)


def square_sum(values):
    widened = values.astype(jnp.float32)
    return jnp.sum(widened * widened, axis=-1, keepdims=True)


def matmul(left, right):
    return jnp.dot(left, right, preferred_element_type=jnp.float32)


def on_device(
    stream,
    in_weight,
    pool_weight,
    pool_scale,
    out_weight,
    mix_gain,
    ffn_gain,
    gate_weight,
    up_weight,
    down_weight,
):
    tp, fs = lax.axis_size("tp"), lax.axis_size("fs")
    t, z = lax.axis_index("tp"), lax.axis_index("fs")
    tokens, width = stream.shape
    features = tp * width
    local_groups, group_dim = pool_weight.shape[:2]

    pieces = {0: stream}
    bit = tp // 2
    while bit:
        pieces.update({m | bit: swap(piece, "tp", bit) for m, piece in list(pieces.items())})
        bit //= 2
    in_rows = gather_planes(in_weight).reshape(features, in_weight.shape[1])
    out_all = gather_planes(out_weight)
    gate_cols = gather_hidden(gate_weight).reshape(features, gate_weight.shape[1])
    up_cols = gather_hidden(up_weight).reshape(features, up_weight.shape[1])
    down_rows = gather_hidden(down_weight)

    out_blocks = {
        m: part(out_all, t ^ m, tp) if m == 0 else swap(part(out_all, t ^ m, tp), "tp", m)
        for m in range(tp)
    }

    scale = lax.rsqrt(sum(square_sum(piece) for piece in pieces.values()) / features + epsilon)
    pooled = 0.0
    for m, piece in pieces.items():
        gain = part(mix_gain, t ^ m, tp).astype(jnp.float32)
        normed = (piece.astype(jnp.float32) * scale * gain).astype(jnp.bfloat16)
        pooled = pooled + matmul(normed, part(in_rows, t ^ m, tp))
    pooled_in = pooled.astype(jnp.bfloat16)

    inside, counts = window_tables(t * local_groups, local_groups, SEQ, GROUPS)
    group_cols = []
    for g in range(local_groups):
        one = pooled_in[:, g * group_dim:(g + 1) * group_dim].reshape(-1, SEQ, group_dim)
        sums = jnp.einsum(
            "ts,nsc->ntc", inside[g].astype(jnp.bfloat16), one, preferred_element_type=jnp.float32
        )
        contrast = (sums / counts[g][None, :, None] - one.astype(jnp.float32)).astype(jnp.bfloat16)
        group_cols.append(matmul(contrast.reshape(tokens, group_dim), pool_weight[g]))
    group_out = (
        jnp.concatenate(group_cols, axis=1) * pool_scale.astype(jnp.float32)
    ).astype(jnp.bfloat16)

    mixer_sum = 0.0
    for m in range(tp):
        block = group_out if m == 0 else swap(group_out, "tp", m)
        rows = out_blocks[m].transpose(1, 0, 2).reshape(block.shape[1], width)
        mixer_sum = mixer_sum + matmul(block, rows)
    middle = (stream.astype(jnp.float32) + mixer_sum).astype(jnp.bfloat16)

    first = (t & ~1) | (z & 1)
    got = jnp.stack([regroup(middle, mask, False) for mask in range(tp)])
    full = jnp.concatenate(
        [lax.dynamic_index_in_dim(got, b ^ first, keepdims=False) for b in range(tp)], axis=1
    ).astype(jnp.float32)
    scale = lax.rsqrt(square_sum(full) / features + epsilon)
    normed_ffn = (full * scale * ffn_gain.astype(jnp.float32)).astype(jnp.bfloat16)
    gate_acts = matmul(normed_ffn, gate_cols)
    up_acts = matmul(normed_ffn, up_cols)
    hidden = (jax.nn.silu(gate_acts) * up_acts).astype(jnp.bfloat16)

    total = middle.astype(jnp.float32)
    for mask in range(tp):
        cols = part(down_rows, first ^ mask, tp).transpose(1, 0, 2).reshape(hidden.shape[1], width)
        product = matmul(hidden, cols).astype(jnp.bfloat16)
        total = total + regroup(product, mask, True).astype(jnp.float32)
    return total.astype(jnp.bfloat16)


def solution(mesh):
    return jax.shard_map(
        on_device,
        mesh=mesh,
        in_specs=(
            P(("rep", "fs"), "tp"),
            P("fs", "tp"),
            P("tp", None, None),
            P("tp"),
            P("tp", "fs"),
            P(),
            P(),
            P("fs", "tp"),
            P("fs", "tp"),
            P("tp", "fs"),
        ),
        out_specs=P(("rep", "fs"), "tp"),
        check_vma=False,
    )
```

```python
import functools

import jax
import jax.numpy as jnp
from jax import lax
from jax.experimental import pallas as pl
from jax.experimental.pallas import tpu as pltpu
from jax.sharding import PartitionSpec as P


GROUPS = 8
SEQ = 128
MAX_SENDS = 8
epsilon = 1e-06


def swap(values, axis, mask):
    return lax.ppermute(values, axis, [(i, i ^ mask) for i in range(lax.axis_size(axis))])


def regroup(values, mask, inverse):
    tp, fs = lax.axis_size("tp"), lax.axis_size("fs")
    edges = []
    for z in range(fs):
        for t in range(tp):
            to_z = (z & ~1) | ((t & 1) ^ (mask & 1))
            to_t = (((t >> 1) ^ (mask >> 1)) << 1) | (z & 1)
            edge = (z * tp + t, to_z * tp + to_t)
            edges.append(edge[::-1] if inverse else edge)
    return lax.ppermute(values, ("fs", "tp"), edges)


def put(buffer, piece, index):
    lead = len(index)
    piece = piece.reshape((1,) * lead + buffer.shape[lead:])
    return lax.dynamic_update_slice(buffer, piece, tuple(index) + (0,) * (buffer.ndim - lead))


def part(values, index, count):
    rows = values.shape[0] // count
    return lax.dynamic_slice_in_dim(values, index * rows, rows, axis=0)


def plane_pieces(shard):
    fs, rep = lax.axis_size("fs"), lax.axis_size("rep")
    mine = part(shard, lax.axis_index("rep"), rep)
    pieces = {}
    for s in range(1, fs):
        got = swap(mine, "fs", s)
        for q in range(rep):
            pieces[s, q] = got if q == 0 else swap(got, "rep", q)
    return pieces


def gather_planes(shard):
    fs, rep = lax.axis_size("fs"), lax.axis_size("rep")
    z, r = lax.axis_index("fs"), lax.axis_index("rep")
    if fs > MAX_SENDS:
        return lax.all_gather(shard, "fs")
    local = shard.reshape(1, rep, shard.shape[0] // rep, shard.shape[1])
    buffer = jnp.broadcast_to(local, (fs,) + local.shape[1:])
    for (s, q), piece in plane_pieces(shard).items():
        buffer = put(buffer, piece, (z ^ s, r ^ q))
    return buffer.reshape(fs, shard.shape[0], shard.shape[1])


def hidden_parts(shard):
    rep = lax.axis_size("rep")
    z, r, c = lax.axis_index("fs"), lax.axis_index("rep"), lax.axis_index("tp") & 1
    same_core = c == (z & 1)
    other = swap(shard, "tp", 1)
    own_part, other_part = part(shard, c * rep + r, 2 * rep), part(other, c * rep + r, 2 * rep)
    even = jnp.where(same_core, own_part, other_part)
    odd = jnp.where(same_core, other_part, own_part)
    return even, odd, shard, other


def hidden_pieces(parts):
    even, odd = parts[:2]
    fs, rep = lax.axis_size("fs"), lax.axis_size("rep")
    pieces = {}
    for s in range(1, fs):
        got = swap(odd if s & 1 else even, "fs", s)
        for q in range(rep):
            piece = got if q == 0 else swap(got, "rep", q)
            pieces[s, 0, q] = piece
            pieces[s, 1, q] = swap(piece, "tp", 1)
    return pieces


def own_block(parts):
    c, z = lax.axis_index("tp") & 1, lax.axis_index("fs")
    return jnp.where(c == (z & 1), parts[2], parts[3])


def gather_hidden(parts):
    even, odd, shard, _ = parts
    fs, rep = lax.axis_size("fs"), lax.axis_size("rep")
    z, r, c = lax.axis_index("fs"), lax.axis_index("rep"), lax.axis_index("tp") & 1
    if fs > MAX_SENDS:
        sends = jnp.stack([odd if s & 1 else even for s in range(fs)])
        sends = jnp.where((z & 1) == 0, sends, jnp.roll(sends, 1, axis=0))
        got = lax.all_to_all(sends, "fs", 0, 0, tiled=True)
        got = lax.all_gather(got, "rep", axis=1)
        both = jnp.stack([got, swap(got, "tp", 1)], axis=1)
        both = jnp.where(c == 0, both, jnp.roll(both, 1, axis=1))
        return both.reshape(fs, shard.shape[0], shard.shape[1])
    local = own_block(parts).reshape((1, 2, rep) + even.shape)
    buffer = jnp.broadcast_to(local, (fs,) + local.shape[1:])
    for (s, e, q), piece in hidden_pieces(parts).items():
        buffer = put(buffer, piece, (z ^ s, c ^ e, r ^ q))
    return buffer.reshape(fs, shard.shape[0], shard.shape[1])


def rows_at(start, count, multiple):
    return pl.ds(pl.multiple_of(start, multiple), count)


def local_call(body, outs, scratch, place, operands):
    in_specs = [pl.BlockSpec(memory_space=pltpu.SMEM)]
    in_specs += [pl.BlockSpec(memory_space=pltpu.VMEM)] * len(operands)
    return pl.pallas_call(
        body,
        out_shape=outs,
        in_specs=in_specs,
        out_specs=jax.tree.map(lambda _: pl.BlockSpec(memory_space=pltpu.VMEM), outs),
        scratch_shapes=scratch,
    )(place, *operands)


def mixer_kernel(tp, rep, keys, place, *refs):
    streams, refs = refs[:tp], refs[tp:]
    gain, own, refs = refs[0], refs[1], refs[2:]
    pieces, refs = refs[: len(keys)], refs[len(keys):]
    pool_weight, pool_scale, out, weight, gains = refs
    z, t, r = place[0], place[1], place[2]
    tokens, width = streams[0].shape
    rows = own.shape[0]
    share = rows // rep
    weight[rows_at(z * rows, rows, rows), :] = own[...]
    for (s, q), piece in zip(keys, pieces):
        weight[rows_at((z ^ s) * rows + (r ^ q) * share, share, share), :] = piece[...]
    gains[...] = gain[...].astype(jnp.float32)
    squares = sum(square_sum(piece[...]) for piece in streams)
    scale = lax.rsqrt(squares / (tp * width) + epsilon)
    pooled = jnp.zeros((tokens, own.shape[1]), jnp.float32)
    for m, piece in enumerate(streams):
        block = t ^ m
        normed = piece[...].astype(jnp.float32) * scale * gains[pl.ds(block, 1), :]
        pooled += matmul(
            normed.astype(jnp.bfloat16), weight[rows_at(block * width, width, width), :]
        )
    pooled = pooled.astype(jnp.bfloat16)
    local_groups, group_dim = pool_weight.shape[:2]
    query = lax.broadcasted_iota(jnp.int32, (SEQ, SEQ), 0)
    earlier = lax.broadcasted_iota(jnp.int32, (SEQ, SEQ), 1)
    for g in range(local_groups):
        reach = lax.shift_left(
            jnp.int32(2), lax.div(4 * (t * local_groups + g), jnp.int32(GROUPS))
        )
        inside = ((earlier <= query) & (earlier > query - reach)).astype(jnp.bfloat16)
        counts = jnp.minimum(query[:, :1] + 1, reach).astype(jnp.float32)
        cols = slice(g * group_dim, (g + 1) * group_dim)
        for n in range(tokens // SEQ):
            one = pooled[n * SEQ:(n + 1) * SEQ, cols]
            contrast = matmul(inside, one) / counts - one.astype(jnp.float32)
            mixed = matmul(contrast.astype(jnp.bfloat16), pool_weight[g])
            out[n * SEQ:(n + 1) * SEQ, cols] = (
                mixed * pool_scale[:, cols].astype(jnp.float32)
            ).astype(jnp.bfloat16)


def fill(weight, own, keys, pieces, place):
    z, c, r = place[0], place[1] & 1, place[2]
    rows, share = own.shape[0], pieces[0].shape[0]
    rep = rows // (2 * share)
    weight[rows_at(z * rows, rows, rows), :] = own[...]
    for (s, e, q), piece in zip(keys, pieces):
        start = (z ^ s) * rows + ((c ^ e) * rep + (r ^ q)) * share
        weight[rows_at(start, share, share), :] = piece[...]


def gate_kernel(tp, keys, place, *refs):
    streams, refs = refs[:tp], refs[tp:]
    gain, own, refs = refs[0], refs[1], refs[2:]
    pieces, refs = refs[: len(keys)], refs[len(keys):]
    normed, acts, weight, gains = refs
    width = streams[0].shape[1]
    first = (place[1] & ~1) | (place[0] & 1)
    gains[...] = gain[...].astype(jnp.float32)
    squares = sum(square_sum(piece[...]) for piece in streams)
    scale = lax.rsqrt(squares / (tp * width) + epsilon)
    for m, piece in enumerate(streams):
        block = first ^ m
        normed[:, rows_at(block * width, width, width)] = (
            piece[...].astype(jnp.float32) * scale * gains[pl.ds(block, 1), :]
        ).astype(jnp.bfloat16)
    fill(weight, own, keys, pieces, place)
    acts[...] = matmul(normed[...], weight[...])


def up_kernel(keys, place, normed, acts, own, *refs):
    pieces, (hidden, weight) = refs[: len(keys)], refs[len(keys):]
    fill(weight, own, keys, pieces, place)
    gate = acts[...]
    hidden[...] = (
        gate / (1.0 + jnp.exp(-gate)) * matmul(normed[...], weight[...])
    ).astype(jnp.bfloat16)


def down_kernel(turns, keys, place, hidden, *refs):
    blocks, refs = refs[: len(keys)], refs[len(keys):]
    outs, (weight,) = refs[: len(turns)], refs[len(turns):]
    c, r = place[1] & 1, place[2]
    flip = (place[0] ^ place[1]) & ~1
    for s in turns:
        whole = [block for key, block in zip(keys, blocks) if key == (s,)]
        parts = [(key, block) for key, block in zip(keys, blocks) if key[0] == s and len(key) > 1]
        if not whole:
            share = parts[0][1].shape[0]
            rep = weight.shape[0] // (2 * share)
            for (_, e, q), block in parts:
                start = ((c ^ e) * rep + (r ^ q)) * share
                weight[rows_at(start, share, share), :] = block[...]
        product = matmul(hidden[...], whole[0][...] if whole else weight[...])
        product = product.astype(jnp.bfloat16)
        for mask, out in zip(turns, outs):

            @pl.when((mask ^ flip) == s)
            def _():
                out[...] = product


def window_tables(first_group, group_count, seq_len, total_groups):
    group_ids = first_group + jnp.arange(group_count, dtype=jnp.int32)
    reaches = jnp.left_shift(jnp.int32(2), 4 * group_ids // total_groups)
    query_pos = jnp.arange(seq_len, dtype=jnp.int32)[:, None]
    earlier = jnp.arange(seq_len, dtype=jnp.int32)[None, :]
    inside = (earlier <= query_pos)[None] & (
        earlier[None] > query_pos[None] - reaches[:, None, None]
    )
    counts = jnp.minimum(query_pos[:, 0][None, :] + 1, reaches[:, None]).astype(jnp.float32)
    return (inside, counts)


def square_sum(values):
    widened = values.astype(jnp.float32)
    return jnp.sum(widened * widened, axis=-1, keepdims=True)


def matmul(left, right):
    return jnp.dot(left, right, preferred_element_type=jnp.float32)


def layer(
    stream,
    in_weight,
    pool_weight,
    pool_scale,
    out_weight,
    mix_gain,
    ffn_gain,
    gate_weight,
    up_weight,
    down_weight,
):
    tp, fs = lax.axis_size("tp"), lax.axis_size("fs")
    t, z = lax.axis_index("tp"), lax.axis_index("fs")
    tokens, width = stream.shape
    features = tp * width
    local_groups, group_dim = pool_weight.shape[:2]

    pairs = fs == tp and tp == 4
    place = jnp.stack([z, t, lax.axis_index("rep")]).astype(jnp.int32)
    gate_parts = hidden_parts(gate_weight)
    early = (gate_parts, stream, mix_gain, ffn_gain, pool_scale, t, in_weight, out_weight)
    gate_parts, own_stream, mix_gain, ffn_gain, pool_scale, late_t, own_in, _ = (
        lax.optimization_barrier(early)
    )
    pieces = {0: stream}
    bit = tp // 2
    while bit:
        pieces.update({m | bit: swap(piece, "tp", bit) for m, piece in list(pieces.items())})
        bit //= 2
    pieces[0] = own_stream

    if pairs:
        in_pieces = plane_pieces(in_weight)
        operands = [pieces[m] for m in range(tp)] + [mix_gain.reshape(tp, width), own_in]
        operands += list(in_pieces.values()) + [pool_weight, pool_scale.reshape(1, -1)]
        group_out = local_call(
            functools.partial(mixer_kernel, tp, lax.axis_size("rep"), list(in_pieces)),
            jax.ShapeDtypeStruct((tokens, in_weight.shape[1]), jnp.bfloat16),
            [
                pltpu.VMEM((features, in_weight.shape[1]), jnp.bfloat16),
                pltpu.VMEM((tp, width), jnp.float32),
            ],
            place,
            operands,
        )
    else:
        in_rows = gather_planes(in_weight).reshape(features, in_weight.shape[1])
        scale = lax.rsqrt(sum(square_sum(piece) for piece in pieces.values()) / features + epsilon)
        pooled = 0.0
        for m, piece in pieces.items():
            gain = part(mix_gain, t ^ m, tp).astype(jnp.float32)
            normed = (piece.astype(jnp.float32) * scale * gain).astype(jnp.bfloat16)
            pooled = pooled + matmul(normed, part(in_rows, t ^ m, tp))
        pooled_in = pooled.astype(jnp.bfloat16)
        inside, counts = window_tables(late_t * local_groups, local_groups, SEQ, GROUPS)
        group_cols = []
        for g in range(local_groups):
            one = pooled_in[:, g * group_dim:(g + 1) * group_dim].reshape(-1, SEQ, group_dim)
            sums = jnp.einsum(
                "ts,nsc->ntc",
                inside[g].astype(jnp.bfloat16),
                one,
                preferred_element_type=jnp.float32,
            )
            contrast = sums / counts[g][None, :, None] - one.astype(jnp.float32)
            contrast = contrast.astype(jnp.bfloat16).reshape(tokens, group_dim)
            group_cols.append(matmul(contrast, pool_weight[g]))
        group_out = (
            jnp.concatenate(group_cols, axis=1) * pool_scale.astype(jnp.float32)
        ).astype(jnp.bfloat16)

    out_all = gather_planes(out_weight)
    out_blocks = {
        m: part(out_all, t, tp) if m == 0 else swap(part(out_all, t ^ m, tp), "tp", m)
        for m in range(tp)
    }
    up_parts, down_parts = hidden_parts(up_weight), hidden_parts(down_weight)

    mixer_sum = 0.0
    for m in range(tp):
        block = group_out if m == 0 else swap(group_out, "tp", m)
        rows = out_blocks[m].transpose(1, 0, 2).reshape(block.shape[1], width)
        mixer_sum = mixer_sum + matmul(block, rows)
    middle = (own_stream.astype(jnp.float32) + mixer_sum).astype(jnp.bfloat16)

    first = (t & ~1) | (z & 1)
    pieces = {mask: regroup(middle, mask, False) for mask in (0, 1)}
    bit = 2
    while bit < tp:
        pieces.update({m | bit: swap(piece, "tp", bit) for m, piece in list(pieces.items())})
        bit *= 2
    total = middle.astype(jnp.float32)
    if pairs:
        hidden_units = gate_weight.shape[1]
        gate_pieces, up_pieces, down_pieces = (
            hidden_pieces(gate_parts), hidden_pieces(up_parts), hidden_pieces(down_parts)
        )
        normed_ffn, gate_acts = local_call(
            functools.partial(gate_kernel, tp, list(gate_pieces)),
            (
                jax.ShapeDtypeStruct((tokens, features), jnp.bfloat16),
                jax.ShapeDtypeStruct((tokens, hidden_units), jnp.float32),
            ),
            [
                pltpu.VMEM((features, hidden_units), jnp.bfloat16),
                pltpu.VMEM((tp, width), jnp.float32),
            ],
            place,
            [pieces[m] for m in range(tp)]
            + [ffn_gain.reshape(tp, width), own_block(gate_parts)]
            + list(gate_pieces.values()),
        )
        hidden = local_call(
            functools.partial(up_kernel, list(up_pieces)),
            jax.ShapeDtypeStruct((tokens, hidden_units), jnp.bfloat16),
            [pltpu.VMEM((features, hidden_units), jnp.bfloat16)],
            place,
            [normed_ffn, gate_acts, own_block(up_parts)] + list(up_pieces.values()),
        )
        down_blocks = {(0,): own_block(down_parts), **down_pieces}
        for turns in ((0, 2), (1, 3)):
            blocks = {key: block for key, block in down_blocks.items() if key[0] in turns}
            products = local_call(
                functools.partial(down_kernel, turns, list(blocks)),
                tuple(jax.ShapeDtypeStruct((tokens, width), jnp.bfloat16) for _ in turns),
                [pltpu.VMEM((hidden_units, width), jnp.bfloat16)],
                place,
                [hidden] + list(blocks.values()),
            )
            for mask, product in zip(turns, products):
                total = total + regroup(product, mask, True).astype(jnp.float32)
        return total.astype(jnp.bfloat16)

    gate_cols = gather_hidden(gate_parts).reshape(features, gate_weight.shape[1])
    up_cols = gather_hidden(up_parts).reshape(features, up_weight.shape[1])
    down_rows = gather_hidden(down_parts)
    got = jnp.stack([pieces[m] for m in range(tp)])
    full = jnp.concatenate(
        [lax.dynamic_index_in_dim(got, b ^ first, keepdims=False) for b in range(tp)], axis=1
    ).astype(jnp.float32)
    scale = lax.rsqrt(square_sum(full) / features + epsilon)
    normed_ffn = (full * scale * ffn_gain.astype(jnp.float32)).astype(jnp.bfloat16)
    gate_acts = matmul(normed_ffn, gate_cols)
    up_acts = matmul(normed_ffn, up_cols)
    hidden = (jax.nn.silu(gate_acts) * up_acts).astype(jnp.bfloat16)
    for mask in range(tp):
        cols = part(down_rows, first ^ mask, tp).transpose(1, 0, 2).reshape(hidden.shape[1], width)
        product = matmul(hidden, cols).astype(jnp.bfloat16)
        total = total + regroup(product, mask, True).astype(jnp.float32)
    return total.astype(jnp.bfloat16)


def solution(mesh):
    return jax.shard_map(
        layer,
        mesh=mesh,
        in_specs=(
            P(("rep", "fs"), "tp"),
            P("fs", "tp"),
            P("tp", None, None),
            P("tp"),
            P("tp", "fs"),
            P(),
            P(),
            P("fs", "tp"),
            P("fs", "tp"),
            P("tp", "fs"),
        ),
        out_specs=P(("rep", "fs"), "tp"),
        check_vma=False,
    )
```
